512 devices in a mesh: ep: 128 (over z, y, core), tp: 4 (over x).
Axes of the slice: x: 4, y: 8, z: 8, core: 2. Of those that a mesh axis runs over, the one named last changes fastest.
Arguments:
- tokens: bfloat16 [2048, 1024], P('ep'), may hold values from -24 to 24
- seq_length: int32 [2048], P('ep'), may hold values from 1024 to 16383
- ret_state: float32 [2048, 4, 128, 256], P('ep', 'tp'), may hold values from -0.6 to 0.6
- norm_in: float32 [1024], replicated, may hold values from 0.1 to 1.9
- w_query: bfloat16 [1024, 512], P(None, 'tp'), may hold values from -0.1875 to 0.1875
- w_key: bfloat16 [1024, 512], P(None, 'tp'), may hold values from -0.1875 to 0.1875
- w_value: bfloat16 [1024, 1024], P(None, 'tp'), may hold values from -0.1875 to 0.1875
- head_gain: float32 [1024], P('tp'), may hold values from 0.1 to 1.9
- w_output: bfloat16 [1024, 1024], P('tp'), may hold values from -0.1875 to 0.1875
- norm_mid: float32 [1024], replicated, may hold values from 0.1 to 1.9
- route_expert: int32 [2048, 2], P('ep'), may hold values from 0 to 63, all different within a row; in each aligned block of 16 rows (0 to 15, 16 to 31, ...) at most 2 rows name the same one
- route_score: float32 [2048, 2], P('ep'), may hold values from -6 to 6
- expert_gate: bfloat16 [128, 1024, 1792], P('ep', None, 'tp'), may hold values from -0.1875 to 0.1875
- expert_up: bfloat16 [128, 1024, 1792], P('ep', None, 'tp'), may hold values from -0.1875 to 0.1875
- expert_down: bfloat16 [128, 1792, 1024], P('ep', 'tp'), may hold values from -0.09375 to 0.09375
Outputs:
- mixed: bfloat16 [2048, 1024], P('ep', 'tp')
The draws below stay inside these ranges and needn't reach their ends.
Inputs may be any that keep to these rules, and one draw needn't show every extreme that they name: `route_expert`: each row names 2 different experts; within the rows of one device no expert is named by more than 2 rows, and some device's rows name one expert exactly 2 times.
All inputs are finite; a program needn't handle non-finite values.
Results may differ from the reference program's by a relative error of at most 0.014.
Values may be sent and summed in bfloat16 or wider, within the bound.
A program may use at most 64 MiB of HBM per device.

```python
import math
import jax
import jax.numpy as jnp
import numpy as np
from jax import lax

D = 1024
HEADS = 4
DK = 128
DV = 256
FF_E = 3584
SPREAD = 2
TOP_K = 2
SEQ_DEV = 16
BATCH = 2048
EXPERTS = 64
CAP = 2
N_EP = 128
N_TP = 4


def draw_tokens(key, part):
    base_key, rough_key = jax.random.split(key, 2)
    column = jnp.arange(D, dtype=jnp.float32) / D
    column_ramp = jnp.exp(jnp.log(0.3) + jnp.log(10.0) * column)
    rough_scale = jax.random.uniform(rough_key, (D,), jnp.float32, 0.5, 1.5)
    base_draw = jnp.clip(jax.random.normal(base_key, (BATCH, D), jnp.float32), -5.0, 5.0)
    return (base_draw * column_ramp * rough_scale).astype(jnp.bfloat16)


def place_ends(array, key, low, largest):
    shape = array.shape
    place = [jax.random.randint(jax.random.fold_in(key, axis), (), 0, shape[axis]) for axis in range(len(shape))]
    array = array.at[tuple(place)].set(low)
    longest = shape.index(max(shape))
    place[longest] = (place[longest] + 1) % shape[longest]
    return array.at[tuple(place)].set(largest)


def block_scale(stream_key, dims, pieces, least, high):
    def one(dim, shards_of):
        steps = jax.random.uniform(jax.random.fold_in(jax.random.fold_in(stream_key, 6), dim), (shards_of,), jnp.float32, least / len(pieces), high / len(pieces))
        return jnp.repeat(jnp.exp(steps), dims[dim] // shards_of).reshape((-1,) + (1,) * (len(dims) - dim - 1))

    level = one(*pieces[0])
    for cut in pieces[1:]:
        level = level * one(*cut)
    return level


def assign_block(rng, own, number, rows, count, top, bound, slope):
    ranking = jax.random.permutation(rng, count)
    heavy_load, usual = shares(count, rows * top, bound, slope, True), shares(count, rows * top, bound, slope, False)
    places = jnp.arange(count)

    def named(lengths, turn):
        used = int((lengths > 0).sum())
        fixed = max(1, used // 4)
        shifted = fixed + (places - fixed + turn * (used - fixed)) % max(1, count - fixed)
        return jnp.zeros((count,), jnp.int32).at[ranking[jnp.where(places < fixed, places, shifted)]].set(jnp.asarray(lengths, jnp.int32))

    lengths = jnp.where(number % 4 == 0, named(heavy_load, number // 4), named(usual, number - number // 4 - 1))
    mixed = jax.random.permutation(jax.random.fold_in(own, 3), count)
    giver, taker = mixed[0:count // 2 * 2:2], mixed[1:count // 2 * 2:2]
    margin = jnp.minimum(lengths[giver] - 1, bound - lengths[taker]) // 2
    margin = jnp.where((giver == ranking[0]) | (taker == ranking[0]) | (lengths[taker] == 0), 0, jnp.maximum(margin, 0))
    shifted = jax.random.randint(jax.random.fold_in(own, 4), (count // 2,), 0, 1 << 20) % (margin + 1)
    lengths = lengths.at[giver].add(-shifted).at[taker].add(shifted)
    items = jnp.searchsorted(jnp.cumsum(lengths), jnp.arange(rows * top), side="right").astype(jnp.int32)
    listing = items.reshape(top, rows).T
    listing = listing[jax.random.permutation(jax.random.fold_in(own, 1), rows)]
    turn = jax.random.randint(jax.random.fold_in(own, 2), (rows, 1), 0, top)
    return jnp.take_along_axis(listing, (jnp.arange(top)[None, :] + turn) % top, axis=1)


def shares(number_of, total, reach, slope, full):
    loads = [(1 << 20) // math.isqrt(rank ** slope) + 1 for rank in range(1, number_of + 1)]
    largest = reach if full else min(reach, max(-(-total // number_of), total * loads[0] // sum(loads)))
    least = 1 if total - largest >= number_of - 1 else 0
    holding, surplus = [largest] + [least] * (number_of - 1), total - largest - least * (number_of - 1)
    while surplus > 0:
        movable = [i for i in range(1, number_of) if holding[i] < largest] or [i for i in range(1, number_of) if holding[i] < reach]
        mass, left = sum([loads[i] for i in movable]), surplus
        for i in movable:
            addition = min(reach - holding[i], max(1, left * loads[i] // mass), surplus)
            holding[i] = holding[i] + addition
            surplus = surplus - addition
    return np.array(holding)


def scatter_about(own_key, extent, width, bound, pieces=(), kind=jnp.bfloat16):
    values = jax.random.normal(own_key, extent, jnp.float32) * width
    if len(pieces) > 0:
        values = block_scale(own_key, extent, pieces, -0.22, 0.18) * values
    return jnp.clip(values, min=-bound, max=bound).astype(kind)


def setup_inputs(seed: int = 0) -> dict:
    splits = jax.random.split(jax.random.key(seed), 16)
    tokens = draw_tokens(jax.random.fold_in(splits[15], 71), 0)
    seq_length = place_ends(jax.random.randint(splits[1], (BATCH,), 1024, 16384), jax.random.fold_in(splits[1], 1), 1024, 16383).astype(jnp.int32)
    ret_state = scatter_about(splits[2], (BATCH, HEADS, DK, DV), 0.1, 0.6, ((0, 128), (1, 4)), jnp.float32)
    norm_in = jnp.clip(1.0 + 0.18 * jax.random.normal(splits[3], (D,), jnp.float32), 0.1, 1.9)
    w_query = scatter_about(splits[4], (D, HEADS * DK), D ** -0.5, 0.1875, ((1, 4),))
    w_key = scatter_about(splits[5], (D, HEADS * DK), D ** -0.5, 0.1875, ((1, 4),))
    w_value = scatter_about(splits[6], (D, HEADS * DV), D ** -0.5, 0.1875, ((1, 4),))
    head_gain = jnp.clip(1.0 + 0.18 * jax.random.normal(splits[7], (HEADS * DV,), jnp.float32), 0.1, 1.9)
    w_output = scatter_about(splits[8], (HEADS * DV, D), (HEADS * DV) ** -0.5, 0.1875, ((0, 4),))
    norm_mid = jnp.clip(1.0 + 0.18 * jax.random.normal(splits[9], (D,), jnp.float32), 0.1, 1.9)
    route_expert_keys = jax.random.split(jax.random.fold_in(splits[10], 1), BATCH // SEQ_DEV)
    route_expert_turns = jax.random.permutation(jax.random.fold_in(splits[10], 3), BATCH // SEQ_DEV)
    route_expert = jax.vmap(lambda own, number: assign_block(jax.random.fold_in(splits[10], 2), own, number, SEQ_DEV, EXPERTS, TOP_K, CAP, 2))(route_expert_keys, route_expert_turns).reshape((BATCH, TOP_K))
    route_score = scatter_about(splits[11], (BATCH, TOP_K), 1.5, 6.0, ((0, 128),), jnp.float32)
    expert_gate = scatter_about(splits[12], (EXPERTS * SPREAD, D, FF_E // SPREAD), D ** -0.5, 0.1875, ((0, 128), (2, 4)))
    expert_up = scatter_about(splits[13], (EXPERTS * SPREAD, D, FF_E // SPREAD), D ** -0.5, 0.1875, ((0, 128), (2, 4)))
    expert_down = scatter_about(splits[14], (EXPERTS * SPREAD, FF_E // SPREAD, D), FF_E ** -0.5, 0.09375, ((0, 128), (1, 4)))
    return dict(tokens=tokens, seq_length=seq_length, ret_state=ret_state, norm_in=norm_in, w_query=w_query, w_key=w_key, w_value=w_value, head_gain=head_gain, w_output=w_output, norm_mid=norm_mid, route_expert=route_expert, route_score=route_score, expert_gate=expert_gate, expert_up=expert_up, expert_down=expert_down)


EPS = 1e-06

def rotate(head_rows, positions):
    half_width = head_rows.shape[-1] // 2
    inverse = 10000.0 ** (-jnp.arange(half_width, dtype=jnp.float32) / half_width)
    angles = positions[:, None] * inverse[None, :]
    cosine = jnp.cos(angles)[:, None, :]
    sine_part = jnp.sin(angles)[:, None, :]
    first_half = head_rows[..., :half_width]
    second = head_rows[..., half_width:]
    return jnp.concatenate([first_half * cosine - second * sine_part, first_half * sine_part + second * cosine], axis=-1)

def expert_block(block_rows, gate_parts, up_parts, down_parts):
    results = []
    for part_index in range(SPREAD):
        gate_sum = jnp.dot(block_rows, gate_parts[part_index], preferred_element_type=jnp.float32)
        up_sum = jnp.dot(block_rows, up_parts[part_index], preferred_element_type=jnp.float32)
        hidden = (jax.nn.silu(gate_sum) * up_sum).astype(jnp.bfloat16)
        lane_width = hidden.shape[1] // N_TP
        totals = jnp.zeros((block_rows.shape[0], D), jnp.float32)
        for lane_index in range(N_TP):
            partial_value = jnp.dot(hidden[:, lane_index * lane_width:(lane_index + 1) * lane_width], down_parts[part_index, lane_index * lane_width:(lane_index + 1) * lane_width], preferred_element_type=jnp.float32).astype(jnp.bfloat16)
            totals = totals + lax.optimization_barrier(partial_value).astype(jnp.float32)
        results.append(totals.astype(jnp.bfloat16))
    return jnp.stack(results)

def reference(tokens, seq_length, ret_state, norm_in, w_query, w_key, w_value, head_gain, w_output, norm_mid, route_expert, route_score, expert_gate, expert_up, expert_down):
    token_f = tokens.astype(jnp.float32)
    normed = (token_f * lax.rsqrt(lax.optimization_barrier(jnp.mean(token_f * token_f, axis=-1, keepdims=True)) + EPS) * norm_in).astype(jnp.bfloat16)
    query_proj = jnp.dot(normed, w_query, preferred_element_type=jnp.float32).astype(jnp.bfloat16)
    key_proj = jnp.dot(normed, w_key, preferred_element_type=jnp.float32).astype(jnp.bfloat16)
    value_proj = jnp.dot(normed, w_value, preferred_element_type=jnp.float32).astype(jnp.bfloat16)
    positions = seq_length.astype(jnp.float32)
    q_rot = rotate(query_proj.astype(jnp.float32).reshape(BATCH, HEADS, DK), positions)
    k_rot = rotate(key_proj.astype(jnp.float32).reshape(BATCH, HEADS, DK), positions) * DK ** (-0.5)
    value_rows = value_proj.astype(jnp.float32).reshape(BATCH, HEADS, DV)
    decay_rate = 1.0 - jnp.exp2(-2.0 - 2.0 * jnp.arange(HEADS, dtype=jnp.float32))
    carried = jnp.einsum('bhd,bhde->bhe', q_rot, ret_state, precision=lax.Precision.HIGHEST)
    within = lax.optimization_barrier(jnp.sum(q_rot * k_rot, axis=-1, keepdims=True)) * value_rows
    retained = decay_rate[None, :, None] * carried + within
    centre = lax.optimization_barrier(jnp.mean(retained, axis=-1, keepdims=True))
    variance = lax.optimization_barrier(jnp.mean(jnp.square(retained - centre), axis=-1, keepdims=True))
    ret_out = ((retained - centre) * lax.rsqrt(variance + EPS)).reshape(BATCH, HEADS * DV)
    ret_out = (ret_out * head_gain).astype(jnp.bfloat16)
    span = HEADS * DV // N_TP
    attended = jnp.zeros((BATCH, D), jnp.float32)
    for lane_index in range(N_TP):
        partial_value = jnp.dot(ret_out[:, lane_index * span:(lane_index + 1) * span], w_output[lane_index * span:(lane_index + 1) * span], preferred_element_type=jnp.float32).astype(jnp.bfloat16)
        attended = attended + lax.optimization_barrier(partial_value).astype(jnp.float32)
    resid = (token_f + attended).astype(jnp.bfloat16)
    resid_f = resid.astype(jnp.float32)
    mid = (resid_f * lax.rsqrt(lax.optimization_barrier(jnp.mean(resid_f * resid_f, axis=-1, keepdims=True)) + EPS) * norm_mid).astype(jnp.bfloat16)
    flat_rows = route_expert.reshape(N_EP, SEQ_DEV * TOP_K)
    onehot = (flat_rows[..., None] == jnp.arange(EXPERTS, dtype=jnp.int32)[None, None, :]).astype(jnp.int32)
    rank_index = lax.optimization_barrier(jnp.sum((jnp.cumsum(onehot, axis=1) - onehot) * onehot, axis=2)).astype(jnp.int32)
    slot_index = (jnp.arange(N_EP, dtype=jnp.int32)[:, None] * CAP + rank_index).reshape(-1)
    token_index = (jnp.arange(BATCH * TOP_K, dtype=jnp.int32) // TOP_K).astype(jnp.int32)
    expert_index = flat_rows.reshape(-1)
    buffer = jnp.zeros((EXPERTS, N_EP * CAP, D), jnp.bfloat16).at[expert_index, slot_index].set(mid[token_index])
    gate_parts = expert_gate.reshape(EXPERTS, SPREAD, D, FF_E // SPREAD)
    up_parts = expert_up.reshape(EXPERTS, SPREAD, D, FF_E // SPREAD)
    down_parts = expert_down.reshape(EXPERTS, SPREAD, FF_E // SPREAD, D)
    results = lax.map(lambda packed: expert_block(packed[0], packed[1], packed[2], packed[3]), (buffer, gate_parts, up_parts, down_parts))
    picked = results[expert_index, :, slot_index, :]
    summed = lax.optimization_barrier(jnp.sum(picked.astype(jnp.float32), axis=1)).astype(jnp.bfloat16)
    summed = lax.optimization_barrier(summed).astype(jnp.float32).reshape(BATCH, TOP_K, D)
    weights = jax.nn.softmax(route_score, axis=-1)
    expert_mix = lax.optimization_barrier(jnp.sum(weights[..., None] * summed, axis=1))
    return (resid_f + expert_mix).astype(jnp.bfloat16)
```

```python
import functools

import jax
import jax.numpy as jnp
from jax import lax
from jax.experimental import pallas as pl
from jax.experimental.pallas import tpu as pltpu
from jax.sharding import PartitionSpec as P

EPS = 1e-06
MESH = pl.DeviceIdType.MESH
F32 = jnp.float32
BF16 = jnp.bfloat16


def dot(a, b):
    return jnp.dot(a, b, preferred_element_type=F32)


def dot_rows(a, b):
    return lax.dot_general(a, b, (((0,), (0,)), ((), ())), preferred_element_type=F32)


def split(x):
    high = x.astype(BF16)
    return high, (x - high.astype(F32)).astype(BF16)


def to_blocks(x):
    rows = x.shape[0]
    return [x[:, 128 * h : 128 * (h + 1)].reshape(rows // 2, 2, 128) for h in range(2)]


def from_blocks(ref):
    blocks = ref.shape[1]
    return jnp.concatenate([ref[h].reshape(2 * blocks, 128) for h in range(2)], axis=1)


def kernel(
    n_ep,
    n_tp,
    tokens_h, seq_h, norm_in_h, wq_h, wk_h, wv_h, state_h, gain_h, wo_h, norm_mid_h,
    route_h, score_h, gate_h, up_h, down_h,
    out_ref,
    tokens, seq, norm_in, wq, wk, wv, state, gain, wo, norm_mid, route, score, gate, up, down,
    carried, a_send, a_recv, b_send, rows, hidden, own, d_send, d_recv, x_send, x_recv, e_send, e_recv,
    load_sem, a_ssem, a_rsem, b_ssem, b_rsem, g_ssem, g_rsem, f_ssem, f_rsem, d_ssem, d_rsem,
    x_ssem, x_rsem, e_ssem, e_rsem,
):
    chips = n_ep // 2
    ep = lax.axis_index("ep")
    tp = lax.axis_index("tp")
    chip = ep // 2
    core = lax.rem(ep, 2)
    other = 1 - core

    def peer(d):
        return lax.rem(tp + d, n_tp)

    def far(r):
        return lax.rem(chip + r, chips)

    sources = (tokens_h, seq_h, norm_in_h, wq_h, wk_h, wv_h, state_h, gain_h, wo_h, norm_mid_h,
               route_h, score_h, gate_h, up_h, down_h)
    places = (tokens, seq, norm_in, wq, wk, wv, state, gain, wo, norm_mid, route, score, gate, up, down)
    loads = [pltpu.make_async_copy(s, p, load_sem.at[i]) for i, (s, p) in enumerate(zip(sources, places))]
    (l_tokens, l_seq, l_norm_in, l_wq, l_wk, l_wv, l_state, l_gain, l_wo, l_norm_mid, l_route, l_score,
     l_gate, l_up, l_down) = loads
    for load in (l_tokens, l_norm_in, l_seq, l_wq, l_wk, l_wv, l_route, l_score, l_state, l_gain, l_wo,
                 l_norm_mid, l_gate, l_up, l_down):
        load.start()

    barrier = pltpu.get_barrier_semaphore()

    def greet(r, carry):
        pl.semaphore_signal(barrier, inc=1, device_id={"ep": far(r) * 2 + core, "tp": tp}, device_id_type=MESH)
        return carry

    lax.fori_loop(1, chips, greet, 0)
    for d in range(1, n_tp):
        pl.semaphore_signal(barrier, inc=1, device_id={"ep": ep, "tp": peer(d)}, device_id_type=MESH)
    pl.semaphore_signal(barrier, inc=1, device_id={"ep": chip * 2 + other, "tp": tp}, device_id_type=MESH)

    l_tokens.wait()
    l_norm_in.wait()
    token_f = tokens[...].astype(F32)
    normed = (
        token_f * lax.rsqrt(jnp.mean(token_f * token_f, axis=-1, keepdims=True) + EPS) * norm_in[...]
    ).astype(BF16)
    l_seq.wait()
    l_route.wait()
    l_score.wait()
    n_rows = token_f.shape[0]
    sub = lax.broadcasted_iota(jnp.int32, (n_rows, n_rows), 0)
    lane = lax.broadcasted_iota(jnp.int32, (n_rows, n_rows), 1)
    positions = jnp.sum(jnp.where(sub == lane, seq[...].astype(F32), 0.0), axis=1, keepdims=True)
    key_lane = lax.broadcasted_iota(jnp.int32, (n_rows, 128), 1)
    pair = lax.rem(key_lane, 64).astype(F32)
    angles = positions * jnp.exp(pair * (-jnp.log(10000.0) / 64.0))
    cosine = jnp.cos(angles)
    sine = jnp.where(key_lane < 64, -1.0, 1.0) * jnp.sin(angles)

    experts = chips
    expert_lane = lax.broadcasted_iota(jnp.int32, (n_rows, 2 * experts), 1)
    choice = [route[:, k : k + 1] for k in range(2)]
    named = [(expert_lane == c).astype(F32) for c in choice]
    earlier = dot((lane < sub).astype(BF16), (named[0] + named[1]).astype(BF16))
    picked = []
    for k in range(2):
        rank = jnp.sum(earlier * named[k], axis=1, keepdims=True).astype(jnp.int32)
        picked.append((expert_lane == choice[k] * 2 + rank).astype(F32))
    placing = (picked[0] + picked[1]).astype(BF16)
    top = jnp.max(score[...], axis=1, keepdims=True)
    grown = jnp.exp(score[...] - top)
    weights = grown / jnp.sum(grown, axis=1, keepdims=True)
    combine = picked[0] * weights[:, 0:1] + picked[1] * weights[:, 1:2]
    combine_high, combine_low = split(combine)

    def rotate(x):
        return x * cosine + pltpu.roll(x, 64, 1) * sine

    l_wq.wait()
    q_rot = rotate(dot(normed, wq[...]).astype(BF16).astype(F32))
    l_wk.wait()
    k_rot = rotate(dot(normed, wk[...]).astype(BF16).astype(F32)) * (128.0 ** -0.5)
    l_wv.wait()
    value_rows = dot(normed, wv[...]).astype(BF16).astype(F32)
    within = jnp.sum(q_rot * k_rot, axis=-1, keepdims=True) * value_rows
    q_cols = q_rot.T
    l_state.wait()
    for b in range(n_rows):
        carried[b : b + 1, :] = jnp.sum(q_cols[:, b : b + 1] * state[b, 0], axis=0, keepdims=True)
    head = jnp.full((1, 1), tp, jnp.int32).astype(F32)
    decay = 1.0 - jnp.exp2(-2.0 - 2.0 * head)
    retained = decay * carried[...] + within
    centred = retained - jnp.mean(retained, axis=-1, keepdims=True)
    variance = jnp.mean(centred * centred, axis=-1, keepdims=True)
    l_gain.wait()
    ret_out = (centred * lax.rsqrt(variance + EPS) * gain[...]).astype(BF16)
    l_wo.wait()
    width = out_ref.shape[1]
    mine = pl.ds(pl.multiple_of(tp * width, 128), width)

    order = [2, 1, 3]
    for d in order:
        columns = pl.ds(pl.multiple_of(peer(d) * width, 128), width)
        a_send[d] = dot(ret_out, wo[:, columns]).astype(BF16)
    own_part = dot(ret_out, wo[:, mine]).astype(BF16).astype(F32)

    pl.semaphore_wait(barrier, chips - 1 + n_tp - 1 + 1)
    a_copies = {}
    for d in order:
        a_copies[d] = pltpu.make_async_remote_copy(
            src_ref=a_send.at[d], dst_ref=a_recv.at[d], send_sem=a_ssem.at[d], recv_sem=a_rsem.at[d],
            device_id={"ep": ep, "tp": peer(d)}, device_id_type=MESH,
        )
        a_copies[d].start()
    attended = own_part
    for d in (1, 3, 2):
        a_copies[d].wait_recv()
        attended = attended + a_recv[d].astype(F32)
    resid = (tokens[:, mine].astype(F32) + attended).astype(BF16)

    packed = dot_rows(placing, resid).astype(BF16)
    for h, part in enumerate(to_blocks(packed)):
        b_send[h] = part

    here = rows.at[tp, core]

    def send_rows(r, carry):
        target = far(r)
        pltpu.make_async_remote_copy(
            src_ref=b_send.at[:, target], dst_ref=here.at[:, r], send_sem=b_ssem, recv_sem=b_rsem,
            device_id={"ep": target * 2 + core, "tp": tp}, device_id_type=MESH,
        ).start()
        return carry

    lax.fori_loop(1, chips, send_rows, 0)
    for h in range(2):
        rows[tp, core, h, 0] = b_send[h, chip]
    rest = pl.ds(1, chips - 1)
    all_rows = pltpu.make_async_remote_copy(
        src_ref=b_send.at[:, rest], dst_ref=here.at[:, rest], send_sem=b_ssem, recv_sem=b_rsem,
        device_id={"ep": ep, "tp": peer(1)}, device_id_type=MESH,
    )
    all_rows.wait_recv()

    g_copies = {}
    for d in order:
        g_copies[d] = pltpu.make_async_remote_copy(
            src_ref=here, dst_ref=here, send_sem=g_ssem.at[d], recv_sem=g_rsem.at[d],
            device_id={"ep": ep, "tp": peer(d)}, device_id_type=MESH,
        )
        g_copies[d].start()

    f_copies = {}

    def forward(d):
        block = rows.at[peer(n_tp - d), core] if d else here
        f_copies[d] = pltpu.make_async_remote_copy(
            src_ref=block, dst_ref=block, send_sem=f_ssem.at[d], recv_sem=f_rsem.at[d],
            device_id={"ep": chip * 2 + other, "tp": tp}, device_id_type=MESH,
        )
        f_copies[d].start()

    forward(0)
    l_norm_mid.wait()
    l_gate.wait()
    l_up.wait()
    squares = [None, None]
    gates = [None, None]
    ups = [None, None]

    def take(side, d):
        source = peer(n_tp - d) if d else tp
        x = from_blocks(rows.at[source, core if side == 0 else other]).astype(F32)
        columns = pl.ds(pl.multiple_of(source * width, 128), width)
        part = jnp.sum(x * x, axis=-1, keepdims=True)
        y = (x * norm_mid[:, columns]).astype(BF16)
        g = dot(y, gate[0, columns, :])
        u = dot(y, up[0, columns, :])
        squares[side] = part if squares[side] is None else squares[side] + part
        gates[side] = g if gates[side] is None else gates[side] + g
        ups[side] = u if ups[side] is None else ups[side] + u

    take(0, 0)
    for d in (1, 3, 2):
        g_copies[d].wait_recv()
        forward(d)
        take(0, d)
    for d in (0, 1, 3, 2):
        f_copies[d].wait_recv()
        take(1, d)
    half = 2 * chips
    for side in range(2):
        scale = lax.rsqrt(squares[side] * (1.0 / (n_tp * width)) + EPS)
        g = gates[side] * scale
        u = ups[side] * scale
        hidden[side] = (g / (1.0 + jnp.exp(-g)) * u).astype(BF16)

    l_down.wait()
    d_copies = {}
    for d in (2, 1, 3, 0):
        columns = pl.ds(pl.multiple_of(peer(d) * width, 128), width)
        d_send[d] = dot(hidden[1], down[0, :, columns]).astype(BF16)
        d_copies[d] = pltpu.make_async_remote_copy(
            src_ref=d_send.at[d], dst_ref=d_recv.at[d], send_sem=d_ssem.at[d], recv_sem=d_rsem.at[d],
            device_id={"ep": chip * 2 + other, "tp": tp}, device_id_type=MESH,
        )
        d_copies[d].start()
        own[d] = dot(hidden[0], down[0, :, columns])
    x_copies = {}
    for d in order:
        d_copies[d].wait_recv()
        x_send[d] = (own[d] + d_recv[d].astype(F32)).astype(BF16)
        x_copies[d] = pltpu.make_async_remote_copy(
            src_ref=x_send.at[d], dst_ref=x_recv.at[d], send_sem=x_ssem.at[d], recv_sem=x_rsem.at[d],
            device_id={"ep": ep, "tp": peer(d)}, device_id_type=MESH,
        )
        x_copies[d].start()
    d_copies[0].wait_recv()
    total = own[0] + d_recv[0].astype(F32)
    for d in (1, 3, 2):
        x_copies[d].wait_recv()
        total = total + x_recv[d].astype(F32)
    for h, part in enumerate(to_blocks(total.astype(BF16))):
        e_send[h] = part

    def send_back(r, carry):
        target = far(chips - r)
        pltpu.make_async_remote_copy(
            src_ref=e_send.at[:, r], dst_ref=e_recv.at[:, chip], send_sem=e_ssem, recv_sem=e_rsem,
            device_id={"ep": target * 2 + core, "tp": tp}, device_id_type=MESH,
        ).start()
        return carry

    lax.fori_loop(1, chips, send_back, 0)
    for h in range(2):
        e_recv[h, chip] = e_send[h, 0]
    all_back = pltpu.make_async_remote_copy(
        src_ref=e_send.at[:, rest], dst_ref=e_recv.at[:, rest], send_sem=e_ssem, recv_sem=e_rsem,
        device_id={"ep": ep, "tp": peer(1)}, device_id_type=MESH,
    )
    all_back.wait_recv()
    back = from_blocks(e_recv)
    mix = dot(combine_high, back) + dot(combine_low, back)
    out_ref[...] = (resid.astype(F32) + mix).astype(BF16)

    all_rows.wait_send()
    all_back.wait_send()
    for d in order:
        a_copies[d].wait_send()
        g_copies[d].wait_send()
        x_copies[d].wait_send()
    for d in range(n_tp):
        f_copies[d].wait_send()
        d_copies[d].wait_send()


def body(
    n_ep, n_tp, tokens, seq_length, ret_state, norm_in, w_query, w_key, w_value, head_gain, w_output,
    norm_mid, route_expert, route_score, expert_gate, expert_up, expert_down,
):
    n_rows, model = tokens.shape
    chips = n_ep // 2
    width = model // n_tp
    args = (
        tokens, seq_length.reshape(1, -1), norm_in.reshape(1, -1), w_query, w_key, w_value, ret_state,
        head_gain.reshape(1, -1), w_output, norm_mid.reshape(1, -1), route_expert, route_score,
        expert_gate, expert_up, expert_down,
    )
    dma = pltpu.SemaphoreType.DMA
    blocks = (2, chips, 2, width // 2)
    scratch = [pltpu.VMEM(a.shape, a.dtype) for a in args] + [
        pltpu.VMEM((n_rows, head_gain.shape[0]), F32),
        pltpu.VMEM((n_tp, n_rows, width), BF16),
        pltpu.VMEM((n_tp, n_rows, width), BF16),
        pltpu.VMEM(blocks, BF16),
        pltpu.VMEM((n_tp, 2) + blocks, BF16),
        pltpu.VMEM((2, 2 * chips, expert_down.shape[1]), BF16),
        pltpu.VMEM((n_tp, 2 * chips, width), F32),
        pltpu.VMEM((n_tp, 2 * chips, width), BF16),
        pltpu.VMEM((n_tp, 2 * chips, width), BF16),
        pltpu.VMEM((n_tp, 2 * chips, width), BF16),
        pltpu.VMEM((n_tp, 2 * chips, width), BF16),
        pltpu.VMEM(blocks, BF16),
        pltpu.VMEM(blocks, BF16),
        dma((len(args),)),
        dma((n_tp,)), dma((n_tp,)),
        dma, dma,
        dma((n_tp,)), dma((n_tp,)),
        dma((n_tp,)), dma((n_tp,)),
        dma((n_tp,)), dma((n_tp,)),
        dma((n_tp,)), dma((n_tp,)),
        dma, dma,
    ]
    return pl.pallas_call(
        functools.partial(kernel, n_ep, n_tp),
        out_shape=jax.ShapeDtypeStruct((n_rows, width), BF16),
        in_specs=[pl.BlockSpec(memory_space=pl.ANY)] * len(args),
        out_specs=pl.BlockSpec(memory_space=pltpu.VMEM),
        scratch_shapes=scratch,
        compiler_params=pltpu.CompilerParams(collective_id=0, has_side_effects=True),
        name="step",
    )(*args)


def solution(mesh):
    placed = (
        P("ep", None),
        P("ep"),
        P("ep", "tp", None, None),
        P(),
        P(None, "tp"),
        P(None, "tp"),
        P(None, "tp"),
        P("tp"),
        P("tp", None),
        P(),
        P("ep", None),
        P("ep", None),
        P("ep", None, "tp"),
        P("ep", None, "tp"),
        P("ep", "tp", None),
    )
    step = functools.partial(body, mesh.shape["ep"], mesh.shape["tp"])
    return jax.shard_map(step, mesh=mesh, in_specs=placed, out_specs=P("ep", "tp"), check_vma=False)
```

```python
import functools

import jax
import jax.numpy as jnp
from jax import lax
from jax.experimental import pallas as pl
from jax.experimental.pallas import tpu as pltpu
from jax.sharding import PartitionSpec as P

EPS = 1e-06
MESH = pl.DeviceIdType.MESH
F32 = jnp.float32
BF16 = jnp.bfloat16


def dot(a, b):
    return jnp.dot(a, b, preferred_element_type=F32)


def dot_cols(a, b):
    return lax.dot_general(a, b, (((1,), (1,)), ((), ())), preferred_element_type=F32)


def dot_rows(a, b):
    return lax.dot_general(a, b, (((0,), (0,)), ((), ())), preferred_element_type=F32)


def split(x):
    high = x.astype(BF16)
    return high, (x - high.astype(F32)).astype(BF16)


def to_blocks(x):
    rows = x.shape[0]
    return [x[:, 128 * h : 128 * (h + 1)].reshape(rows // 2, 2, 128) for h in range(2)]


def from_blocks(ref):
    blocks = ref.shape[1]
    return jnp.concatenate([ref[h].reshape(2 * blocks, 128) for h in range(2)], axis=1)


def ring_order(n_z, n_y):
    def hops(d):
        return min(d[0], n_z - d[0]) + min(d[1], n_y - d[1])

    return sorted(((dz, dy) for dz in range(n_z) for dy in range(n_y)), key=hops)


def kernel(
    n_ep,
    n_tp,
    tokens_h, seq_h, norm_in_h, wq_h, wk_h, wv_h, state_h, gain_h, wo_h, norm_mid_h,
    route_h, score_h, gate_h, up_h, down_h,
    out_ref,
    tokens, seq, norm_in, w_qkv, state, gain, wo, norm_mid, route, score, gate, up, down,
    carried, a_send, a_recv, b_send, rows, own, d_send, d_recv, x_send, x_recv, e_send, e_recv,
    load_sem, line_sem, a_ssem, a_rsem, b_ssem, b_rsem, g_ssem, g_rsem, f_ssem, f_rsem, d_ssem, d_rsem,
    x_ssem, x_rsem, e_ssem, e_rsem,
):
    chips = n_ep // 2
    ep = lax.axis_index("ep")
    tp = lax.axis_index("tp")
    chip = lax.div(ep, 2)
    core = lax.rem(ep, 2)
    other = 1 - core

    def peer(d):
        return lax.rem(tp + d, n_tp)

    n_y = 8 if chips % 8 == 0 else 2
    n_z = chips // n_y
    z = lax.div(chip, n_y)
    y = lax.rem(chip, n_y)
    offsets = ring_order(n_z, n_y)
    near = chips * 5 // 8

    def ahead(dz, dy):
        return lax.rem(z + dz, n_z) * n_y + lax.rem(y + dy, n_y)

    def target(p):
        return ahead(*offsets[p])

    def source(p):
        dz, dy = offsets[p]
        return ahead(n_z - dz, n_y - dy)

    def ep_id(c, co):
        return {"ep": c * 2 + co, "tp": tp}

    def tp_id(d):
        return {"ep": ep, "tp": peer(d)}

    sources = (tokens_h, seq_h, norm_in_h, wq_h, wk_h, wv_h, state_h, gain_h, wo_h, norm_mid_h,
               route_h, score_h, gate_h, up_h, down_h)
    places = (tokens, seq, norm_in, w_qkv.at[:, :128], w_qkv.at[:, 128:256], w_qkv.at[:, 256:], state, gain, wo, norm_mid, route, score, gate, up, down)
    loads = [pltpu.make_async_copy(s, p, load_sem.at[i]) for i, (s, p) in enumerate(zip(sources, places))]
    (l_tokens, l_seq, l_norm_in, l_wq, l_wk, l_wv, l_state, l_gain, l_wo, l_norm_mid, l_route, l_score,
     l_gate, l_up, l_down) = loads
    for load in (l_tokens, l_norm_in, l_seq, l_wq, l_wk, l_wv, l_route, l_score, l_state, l_gain, l_wo,
                 l_norm_mid, l_gate, l_up, l_down):
        load.start()

    barrier = pltpu.get_barrier_semaphore()

    lines = [ahead(0, d) for d in range(1, n_y)] + [ahead(d, 0) for d in range(1, n_z)]
    for d in range(1, n_tp):
        pl.semaphore_signal(barrier, inc=1, device_id=tp_id(d), device_id_type=MESH)
    pl.semaphore_signal(barrier, inc=1, device_id=ep_id(chip, other), device_id_type=MESH)
    for c in lines:
        pl.semaphore_signal(barrier, inc=1, device_id=ep_id(c, core), device_id_type=MESH)

    l_tokens.wait()
    l_norm_in.wait()
    token_f = tokens[...].astype(F32)
    normed = (
        token_f * lax.rsqrt(jnp.mean(token_f * token_f, axis=-1, keepdims=True) + EPS) * norm_in[...]
    ).astype(BF16)
    l_seq.wait()
    n_rows = token_f.shape[0]
    sub = lax.broadcasted_iota(jnp.int32, (n_rows, n_rows), 0)
    lane = lax.broadcasted_iota(jnp.int32, (n_rows, n_rows), 1)

    def column(row):
        return jnp.sum(jnp.where(sub == lane, row.astype(F32), 0.0), axis=1, keepdims=True)

    positions = column(seq[...])
    key_lane = lax.broadcasted_iota(jnp.int32, (n_rows, 128), 1)
    pair = lax.rem(key_lane, 64).astype(F32)
    angles = positions * jnp.exp(pair * (-jnp.log(10000.0) / 64.0))
    cosine = jnp.cos(angles)
    sine = jnp.where(key_lane < 64, -1.0, 1.0) * jnp.sin(angles)

    def rotate(x):
        return x * cosine + pltpu.roll(x, 64, 1) * sine

    l_wq.wait()
    l_wk.wait()
    l_wv.wait()
    projected = dot(normed, w_qkv[...]).astype(BF16).astype(F32)
    q_rot = rotate(projected[:, :128])
    k_rot = rotate(projected[:, 128:256]) * (128.0 ** -0.5)
    value_rows = projected[:, 256:]
    within = jnp.sum(q_rot * k_rot, axis=-1, keepdims=True) * value_rows
    q_cols = q_rot.T
    l_state.wait()
    for b in range(n_rows):
        carried[b : b + 1, :] = jnp.sum(q_cols[:, b : b + 1] * state[b, 0], axis=0, keepdims=True)
    head = jnp.full((1, 1), tp, jnp.int32).astype(F32)
    decay = 1.0 - jnp.exp2(-2.0 - 2.0 * head)
    retained = decay * carried[...] + within
    centred = retained - jnp.mean(retained, axis=-1, keepdims=True)
    variance = jnp.mean(centred * centred, axis=-1, keepdims=True)
    l_gain.wait()
    ret_out = (centred * lax.rsqrt(variance + EPS) * gain[...]).astype(BF16)
    l_wo.wait()
    width = out_ref.shape[1]
    mine = pl.ds(pl.multiple_of(tp * width, 128), width)

    order = [2, 1, 3]
    for d in order:
        columns = pl.ds(pl.multiple_of(peer(d) * width, 128), width)
        a_send[d] = dot(ret_out, wo[:, columns]).astype(BF16)
    own_part = dot(ret_out, wo[:, mine]).astype(BF16).astype(F32)

    pl.semaphore_wait(barrier, n_tp + len(lines))
    for d in range(1, n_z):
        pl.semaphore_signal(line_sem, inc=1, device_id=ep_id(ahead(d, 0), core), device_id_type=MESH)
    a_copies = {}
    for d in order:
        a_copies[d] = pltpu.make_async_remote_copy(
            src_ref=a_send.at[d], dst_ref=a_recv.at[d], send_sem=a_ssem.at[d], recv_sem=a_rsem.at[d],
            device_id=tp_id(d), device_id_type=MESH,
        )
        a_copies[d].start()

    l_route.wait()
    l_score.wait()
    experts = chips
    expert_lane = lax.broadcasted_iota(jnp.int32, (n_rows, 2 * experts), 1)
    choice = [column(route[k : k + 1, :]).astype(jnp.int32) for k in range(2)]
    named = [(expert_lane == c).astype(F32) for c in choice]
    earlier = dot((lane < sub).astype(BF16), (named[0] + named[1]).astype(BF16))
    picked = []
    for k in range(2):
        rank = jnp.sum(earlier * named[k], axis=1, keepdims=True).astype(jnp.int32)
        picked.append((expert_lane == choice[k] * 2 + rank).astype(F32))
    placing = (picked[0] + picked[1]).astype(BF16)
    grown = jnp.exp(score[...] - jnp.max(score[...], axis=0, keepdims=True))
    weights = grown / jnp.sum(grown, axis=0, keepdims=True)
    combine = picked[0] * column(weights[0:1, :]) + picked[1] * column(weights[1:2, :])
    combine_high, combine_low = split(combine)


    attended = own_part
    for d in (1, 3, 2):
        a_copies[d].wait_recv()
        attended = attended + a_recv[d].astype(F32)
    resid = (tokens[:, mine].astype(F32) + attended).astype(BF16)

    packed = dot_rows(placing, resid).astype(BF16)
    for h, part in enumerate(to_blocks(packed)):
        b_send[h] = part

    here = rows.at[tp, core]
    groups = (pl.ds(0, near), pl.ds(near, chips - near))
    pl.semaphore_wait(line_sem, n_z - 1)
    for p in range(chips - 1, 0, -1):
        far = target(p)
        pltpu.make_async_remote_copy(
            src_ref=b_send.at[:, far], dst_ref=here.at[:, p], send_sem=b_ssem, recv_sem=b_rsem.at[int(p >= near)],
            device_id=ep_id(far, core), device_id_type=MESH,
        ).start()
    for h in range(2):
        rows[tp, core, h, 0] = b_send[h, chip]

    def expect(group, recv_sem):
        first, size = ((1, near - 1), (near, chips - near))[group]
        block = here.at[:, pl.ds(first, size)]
        return pltpu.make_async_remote_copy(
            src_ref=block, dst_ref=block, send_sem=b_ssem, recv_sem=recv_sem, device_id=tp_id(1), device_id_type=MESH,
        )

    g_copies, f_copies = {}, {}

    def forward(g, d):
        block = rows.at[peer(n_tp - d) if d else tp, core].at[:, groups[g]]
        f_copies[g, d] = pltpu.make_async_remote_copy(
            src_ref=block, dst_ref=block, send_sem=f_ssem.at[g, d], recv_sem=f_rsem.at[g, d],
            device_id=ep_id(chip, other), device_id_type=MESH,
        )
        f_copies[g, d].start()

    def spread(g):
        expect(g, b_rsem.at[g]).wait_recv()
        block = here.at[:, groups[g]]
        for d in order:
            for side in range(g + 1):
                g_copies[g, d, side] = pltpu.make_async_remote_copy(
                    src_ref=block, dst_ref=block, send_sem=g_ssem.at[g + side, d], recv_sem=g_rsem.at[g + side, d],
                    device_id={"ep": chip * 2 + (other if side else core), "tp": peer(d)}, device_id_type=MESH,
                )
                g_copies[g, d, side].start()
        forward(g, 0)

    sums = {}

    def take(g, side, d):
        lane_group = peer(n_tp - d) if d else tp
        x = from_blocks(rows.at[lane_group, core if side == 0 else other].at[:, groups[g]]).astype(F32)
        columns = pl.ds(pl.multiple_of(lane_group * width, 128), width)
        part = jnp.sum(x * x, axis=-1, keepdims=True)
        y_rows = (x * norm_mid[:, columns]).astype(BF16)
        new = (part, dot_cols(y_rows, gate[0, :, columns]), dot_cols(y_rows, up[0, :, columns]))
        old = sums.get((g, side))
        sums[g, side] = new if old is None else tuple(m + n for m, n in zip(old, new))

    def finish(g, side):
        squares, g_sum, u_sum = sums[g, side]
        scale = lax.rsqrt(squares * (1.0 / (n_tp * width)) + EPS)
        gated = g_sum * scale
        return (gated / (1.0 + jnp.exp(-gated)) * (u_sum * scale)).astype(BF16)

    spread(0)
    l_norm_mid.wait()
    l_gate.wait()
    l_up.wait()
    take(0, 0, 0)
    spread(1)
    take(1, 0, 0)
    for d in (1, 3, 2):
        g_copies[0, d, 0].wait_recv()
        forward(0, d)
        take(0, 0, d)
    f_copies[0, 0].wait_recv()
    take(0, 1, 0)
    f_copies[1, 0].wait_recv()
    take(1, 1, 0)
    for d in (1, 3, 2):
        f_copies[0, d].wait_recv()
        take(0, 1, d)
    for d in (1, 3, 2):
        for side in range(2):
            g_copies[1, d, side].wait_recv()
            take(1, side, d)
    l_down.wait()
    d_copies, x_copies, totals = {}, {}, {}
    spans = [pl.ds(2 * part.start, 2 * part.size) for part in groups]

    def down_dot(both, d):
        columns = pl.ds(pl.multiple_of(peer(d) * width, 128), width)
        product = dot(both, down[0, :, columns])
        half = both.shape[0] // 2
        return product[:half], product[half:]

    both = jnp.concatenate([finish(1, 1), finish(1, 0)], axis=0)
    span = spans[1]
    for d in (2, 1, 3, 0):
        for side, part in enumerate(reversed(down_dot(both, d))):
            if d == 0 and side == 0:
                totals[1] = part
                continue
            x_send[side, d, span] = part.astype(BF16)
            x_copies[1, d, side] = pltpu.make_async_remote_copy(
                src_ref=x_send.at[side, d, span], dst_ref=x_recv.at[side, d, span],
                send_sem=x_ssem.at[1 + side, d], recv_sem=x_rsem.at[1 + side, d],
                device_id={"ep": chip * 2 + (other if side else core), "tp": peer(d)}, device_id_type=MESH,
            )
            x_copies[1, d, side].start()

    both = jnp.concatenate([finish(0, 1), finish(0, 0)], axis=0)
    span = spans[0]
    for d in (2, 1, 3, 0):
        theirs, ours = down_dot(both, d)
        d_send[d, span] = theirs.astype(BF16)
        d_copies[d] = pltpu.make_async_remote_copy(
            src_ref=d_send.at[d, span], dst_ref=d_recv.at[d, span], send_sem=d_ssem.at[d], recv_sem=d_rsem.at[d],
            device_id=ep_id(chip, other), device_id_type=MESH,
        )
        d_copies[d].start()
        own[d, span] = ours
    for d in order:
        d_copies[d].wait_recv()
        x_send[0, d, span] = (own[d, span] + d_recv[d, span].astype(F32)).astype(BF16)
        x_copies[0, d, 0] = pltpu.make_async_remote_copy(
            src_ref=x_send.at[0, d, span], dst_ref=x_recv.at[0, d, span],
            send_sem=x_ssem.at[0, d], recv_sem=x_rsem.at[0, d], device_id=tp_id(d), device_id_type=MESH,
        )
        x_copies[0, d, 0].start()
    d_copies[0].wait_recv()
    totals[0] = own[0, span] + d_recv[0, span].astype(F32)

    def give_back(g):
        span = spans[g]
        total = totals[g]
        for side in range(g, -1, -1):
            for d in (0, 1, 3, 2):
                if (g, d, side) in x_copies:
                    x_copies[g, d, side].wait_recv()
                    total = total + x_recv[side, d, span].astype(F32)
        for h, part in enumerate(to_blocks(total.astype(BF16))):
            e_send[h, groups[g]] = part
        for p in range(groups[g].start + groups[g].size - 1, max(0, groups[g].start - 1), -1):
            pltpu.make_async_remote_copy(
                src_ref=e_send.at[:, p], dst_ref=e_recv.at[:, chip], send_sem=e_ssem, recv_sem=e_rsem,
                device_id=ep_id(source(p), core), device_id_type=MESH,
            ).start()

    give_back(1)
    give_back(0)
    for h in range(2):
        e_recv[h, chip] = e_send[h, 0]
    rest = pl.ds(1, chips - 1)
    all_back = pltpu.make_async_remote_copy(
        src_ref=e_send.at[:, rest], dst_ref=e_recv.at[:, rest], send_sem=e_ssem, recv_sem=e_rsem,
        device_id=tp_id(1), device_id_type=MESH,
    )
    all_back.wait_recv()
    back = from_blocks(e_recv)
    mix = dot(combine_high, back) + dot(combine_low, back)
    out_ref[...] = (resid.astype(F32) + mix).astype(BF16)

    pltpu.make_async_remote_copy(
        src_ref=b_send.at[:, rest], dst_ref=here.at[:, rest], send_sem=b_ssem, recv_sem=b_rsem.at[0],
        device_id=tp_id(1), device_id_type=MESH,
    ).wait_send()
    all_back.wait_send()
    for d in order:
        a_copies[d].wait_send()
    for copies in (g_copies, f_copies, d_copies, x_copies):
        for copy in copies.values():
            copy.wait_send()


def body(
    n_ep, n_tp, tokens, seq_length, ret_state, norm_in, w_query, w_key, w_value, head_gain, w_output,
    norm_mid, route_expert, route_score, expert_gate, expert_up, expert_down,
):
    n_rows, model = tokens.shape
    chips = n_ep // 2
    width = model // n_tp
    args = (
        tokens, seq_length.reshape(1, -1), norm_in.reshape(1, -1), w_query, w_key, w_value, ret_state,
        head_gain.reshape(1, -1), w_output, norm_mid.reshape(1, -1), route_expert.T, route_score.T,
        expert_gate.swapaxes(1, 2), expert_up.swapaxes(1, 2), expert_down,
    )
    dma = pltpu.SemaphoreType.DMA
    blocks = (2, chips, 2, width // 2)
    held = [jax.ShapeDtypeStruct((model, 512), BF16) if a is w_query else a for a in args if a is not w_key and a is not w_value]
    scratch = [pltpu.VMEM(a.shape, a.dtype) for a in held] + [
        pltpu.VMEM((n_rows, head_gain.shape[0]), F32),
        pltpu.VMEM((n_tp, n_rows, width), BF16),
        pltpu.VMEM((n_tp, n_rows, width), BF16),
        pltpu.VMEM(blocks, BF16),
        pltpu.VMEM((n_tp, 2) + blocks, BF16),
        pltpu.VMEM((n_tp, 2 * chips, width), F32),
        pltpu.VMEM((n_tp, 2 * chips, width), BF16),
        pltpu.VMEM((n_tp, 2 * chips, width), BF16),
        pltpu.VMEM((2, n_tp, 2 * chips, width), BF16),
        pltpu.VMEM((2, n_tp, 2 * chips, width), BF16),
        pltpu.VMEM(blocks, BF16),
        pltpu.VMEM(blocks, BF16),
        dma((len(args),)),
        pltpu.SemaphoreType.REGULAR,
        dma((n_tp,)), dma((n_tp,)),
        dma, dma((2,)),
        dma((3, n_tp)), dma((3, n_tp)),
        dma((2, n_tp)), dma((2, n_tp)),
        dma((n_tp,)), dma((n_tp,)),
        dma((3, n_tp)), dma((3, n_tp)),
        dma, dma,
    ]
    return pl.pallas_call(
        functools.partial(kernel, n_ep, n_tp),
        out_shape=jax.ShapeDtypeStruct((n_rows, width), BF16),
        in_specs=[pl.BlockSpec(memory_space=pl.ANY)] * len(args),
        out_specs=pl.BlockSpec(memory_space=pltpu.VMEM),
        scratch_shapes=scratch,
        compiler_params=pltpu.CompilerParams(collective_id=0, has_side_effects=True),
        name="step",
    )(*args)


def solution(mesh):
    placed = (
        P("ep", None),
        P("ep"),
        P("ep", "tp", None, None),
        P(),
        P(None, "tp"),
        P(None, "tp"),
        P(None, "tp"),
        P("tp"),
        P("tp", None),
        P(),
        P("ep", None),
        P("ep", None),
        P("ep", None, "tp"),
        P("ep", None, "tp"),
        P("ep", "tp", None),
    )
    step = functools.partial(body, mesh.shape["ep"], mesh.shape["tp"])
    return jax.shard_map(step, mesh=mesh, in_specs=placed, out_specs=P("ep", "tp"), check_vma=False)
```

```python
import functools

import jax
import jax.numpy as jnp
from jax import lax
from jax.experimental import pallas as pl
from jax.experimental.pallas import tpu as pltpu
from jax.sharding import PartitionSpec as P

EPS = 1e-06
MESH = pl.DeviceIdType.MESH
F32 = jnp.float32
BF16 = jnp.bfloat16


def dot(a, b):
    return jnp.dot(a, b, preferred_element_type=F32)


def dot_cols(a, b):
    return lax.dot_general(a, b, (((1,), (1,)), ((), ())), preferred_element_type=F32)


def dot_rows(a, b):
    return lax.dot_general(a, b, (((0,), (0,)), ((), ())), preferred_element_type=F32)


def split(x):
    high = x.astype(BF16)
    return high, (x - high.astype(F32)).astype(BF16)


def to_blocks(x):
    rows = x.shape[0]
    return [x[:, 128 * h : 128 * (h + 1)].reshape(rows // 2, 2, 128) for h in range(2)]


def from_blocks(ref):
    blocks = ref.shape[1]
    return jnp.concatenate([ref[h].reshape(2 * blocks, 128) for h in range(2)], axis=1)


def ring_order(n_z, n_y):
    def hops(d):
        return min(d[0], n_z - d[0]) + min(d[1], n_y - d[1])

    return sorted(((dz, dy) for dz in range(n_z) for dy in range(n_y)), key=hops)


def kernel(
    n_ep,
    n_tp,
    tokens_h, seq_h, norm_in_h, wq_h, wk_h, wv_h, state_h, gain_h, wo_h, norm_mid_h,
    route_h, score_h, gate_h, up_h, down_h,
    out_ref,
    tokens, seq, norm_in, w_qkv, state, gain, wo, norm_mid, route, score, gate, up, down,
    carried, a_send, a_recv, b_send, rows, own, d_send, d_recv, x_send, x_recv, e_send, e_recv,
    load_sem, line_sem, a_ssem, a_rsem, b_ssem, b_rsem, g_ssem, g_rsem, f_ssem, f_rsem, d_ssem, d_rsem,
    x_ssem, x_rsem, e_ssem, e_rsem,
):
    chips = n_ep // 2
    ep = lax.axis_index("ep")
    tp = lax.axis_index("tp")
    chip = lax.div(ep, 2)
    core = lax.rem(ep, 2)
    other = 1 - core

    def peer(d):
        return lax.rem(tp + d, n_tp)

    n_y = 8 if chips % 8 == 0 else 2
    n_z = chips // n_y
    z = lax.div(chip, n_y)
    y = lax.rem(chip, n_y)
    offsets = ring_order(n_z, n_y)
    near = chips * 5 // 8

    def ahead(dz, dy):
        return lax.rem(z + dz, n_z) * n_y + lax.rem(y + dy, n_y)

    def target(p):
        return ahead(*offsets[p])

    def source(p):
        dz, dy = offsets[p]
        return ahead(n_z - dz, n_y - dy)

    def ep_id(c, co):
        return {"ep": c * 2 + co, "tp": tp}

    def tp_id(d):
        return {"ep": ep, "tp": peer(d)}

    sources = (tokens_h, seq_h, norm_in_h, wq_h, wk_h, wv_h, state_h, gain_h, wo_h, norm_mid_h,
               route_h, score_h, gate_h, up_h, down_h)
    places = (tokens, seq, norm_in, w_qkv.at[:, :128], w_qkv.at[:, 128:256], w_qkv.at[:, 256:], state, gain, wo, norm_mid, route, score, gate, up, down)
    loads = [pltpu.make_async_copy(s, p, load_sem.at[i]) for i, (s, p) in enumerate(zip(sources, places))]
    halves = [pl.ds(0, tokens.shape[0] // 2), pl.ds(tokens.shape[0] // 2, tokens.shape[0] // 2)]
    l_states = [
        pltpu.make_async_copy(state_h.at[half], state.at[half], load_sem.at[len(loads) + i]) for i, half in enumerate(halves)
    ]
    (l_tokens, l_seq, l_norm_in, l_wq, l_wk, l_wv, l_state, l_gain, l_wo, l_norm_mid, l_route, l_score,
     l_gate, l_up, l_down) = loads
    for load in (l_tokens, l_norm_in, l_seq, l_wq, l_wk, l_wv):
        load.start()

    barrier = pltpu.get_barrier_semaphore()

    lines = [ahead(0, d) for d in range(1, n_y)] + [ahead(d, 0) for d in range(1, n_z)]
    for d in range(1, n_tp):
        pl.semaphore_signal(barrier, inc=1, device_id=tp_id(d), device_id_type=MESH)
    pl.semaphore_signal(barrier, inc=1, device_id=ep_id(chip, other), device_id_type=MESH)
    for c in lines:
        pl.semaphore_signal(barrier, inc=1, device_id=ep_id(c, core), device_id_type=MESH)

    for load in (*l_states, l_gain, l_wo):
        load.start()
    l_tokens.wait()
    l_norm_in.wait()
    l_seq.wait()
    l_wq.wait()
    l_wk.wait()
    l_wv.wait()
    token_f = tokens[...].astype(F32)
    row_scale = lax.rsqrt(jnp.mean(token_f * token_f, axis=-1, keepdims=True) + EPS)
    n_rows = token_f.shape[0]
    sub = lax.broadcasted_iota(jnp.int32, (n_rows, n_rows), 0)
    lane = lax.broadcasted_iota(jnp.int32, (n_rows, n_rows), 1)

    def column(row):
        return jnp.sum(jnp.where(sub == lane, row.astype(F32), 0.0), axis=1, keepdims=True)

    positions = column(seq[...])
    key_lane = lax.broadcasted_iota(jnp.int32, (n_rows, 128), 1)
    pair = lax.rem(key_lane, 64).astype(F32)
    angles = positions * jnp.exp(pair * (-jnp.log(10000.0) / 64.0))
    cosine = jnp.cos(angles)
    sine = jnp.where(key_lane < 64, -1.0, 1.0) * jnp.sin(angles)

    def rotate(x):
        return x * cosine + pltpu.roll(x, 64, 1) * sine

    projected = dot((token_f * norm_in[...]).astype(BF16), w_qkv[...]) * row_scale
    q_rot = rotate(projected[:, :128])
    k_rot = rotate(projected[:, 128:256]) * (128.0 ** -0.5)
    value_rows = projected[:, 256:]
    within = jnp.sum(q_rot * k_rot, axis=-1, keepdims=True) * value_rows
    for load in (l_route, l_score, l_norm_mid, l_gate, l_up, l_down):
        load.start()
    q_cols = q_rot.T
    for b in range(n_rows):
        if b % (n_rows // 2) == 0:
            l_states[b // (n_rows // 2)].wait()
        carried[b : b + 1, :] = jnp.sum(q_cols[:, b : b + 1] * state[b, 0], axis=0, keepdims=True)
    head = jnp.full((1, 1), tp, jnp.int32).astype(F32)
    decay = 1.0 - jnp.exp2(-2.0 - 2.0 * head)
    retained = decay * carried[...] + within
    centred = retained - jnp.mean(retained, axis=-1, keepdims=True)
    variance = jnp.mean(centred * centred, axis=-1, keepdims=True)
    l_gain.wait()
    ret_out = (centred * lax.rsqrt(variance + EPS) * gain[...]).astype(BF16)
    l_wo.wait()
    width = out_ref.shape[1]
    mine = pl.ds(pl.multiple_of(tp * width, 128), width)

    order = [2, 1, 3]
    for d in order:
        columns = pl.ds(pl.multiple_of(peer(d) * width, 128), width)
        a_send[d] = dot(ret_out, wo[:, columns]).astype(BF16)
    own_part = dot(ret_out, wo[:, mine]).astype(BF16).astype(F32)

    pl.semaphore_wait(barrier, n_tp + len(lines))
    for d in range(1, n_z):
        pl.semaphore_signal(line_sem, inc=1, device_id=ep_id(ahead(d, 0), core), device_id_type=MESH)
    a_copies = {}
    for d in order:
        a_copies[d] = pltpu.make_async_remote_copy(
            src_ref=a_send.at[d], dst_ref=a_recv.at[d], send_sem=a_ssem.at[d], recv_sem=a_rsem.at[d],
            device_id=tp_id(d), device_id_type=MESH,
        )
        a_copies[d].start()

    l_route.wait()
    l_score.wait()
    experts = chips
    expert_lane = lax.broadcasted_iota(jnp.int32, (n_rows, 2 * experts), 1)
    choice = [column(route[k : k + 1, :]).astype(jnp.int32) for k in range(2)]
    named = [(expert_lane == c).astype(F32) for c in choice]
    earlier = dot((lane < sub).astype(BF16), (named[0] + named[1]).astype(BF16))
    picked = []
    for k in range(2):
        rank = jnp.sum(earlier * named[k], axis=1, keepdims=True).astype(jnp.int32)
        picked.append((expert_lane == choice[k] * 2 + rank).astype(F32))
    placing = (picked[0] + picked[1]).astype(BF16)
    grown = jnp.exp(score[...] - jnp.max(score[...], axis=0, keepdims=True))
    weights = grown / jnp.sum(grown, axis=0, keepdims=True)
    combine = picked[0] * column(weights[0:1, :]) + picked[1] * column(weights[1:2, :])
    combine_high, combine_low = split(combine)


    attended = own_part
    for d in (1, 3, 2):
        a_copies[d].wait_recv()
        attended = attended + a_recv[d].astype(F32)
    resid = (tokens[:, mine].astype(F32) + attended).astype(BF16)

    packed = dot_rows(placing, resid).astype(BF16)
    for h, part in enumerate(to_blocks(packed)):
        b_send[h] = part

    here = rows.at[tp, core]
    groups = (pl.ds(0, near), pl.ds(near, chips - near))
    pl.semaphore_wait(line_sem, n_z - 1)
    for p in range(chips - 1, 0, -1):
        far = target(p)
        pltpu.make_async_remote_copy(
            src_ref=b_send.at[:, far], dst_ref=here.at[:, p], send_sem=b_ssem, recv_sem=b_rsem.at[int(p >= near)],
            device_id=ep_id(far, core), device_id_type=MESH,
        ).start()
    for h in range(2):
        rows[tp, core, h, 0] = b_send[h, chip]

    def expect(group, recv_sem):
        first, size = ((1, near - 1), (near, chips - near))[group]
        block = here.at[:, pl.ds(first, size)]
        return pltpu.make_async_remote_copy(
            src_ref=block, dst_ref=block, send_sem=b_ssem, recv_sem=recv_sem, device_id=tp_id(1), device_id_type=MESH,
        )

    g_copies, f_copies = {}, {}

    def forward(g, d):
        block = rows.at[peer(n_tp - d) if d else tp, core].at[:, groups[g]]
        f_copies[g, d] = pltpu.make_async_remote_copy(
            src_ref=block, dst_ref=block, send_sem=f_ssem.at[g, d], recv_sem=f_rsem.at[g, d],
            device_id=ep_id(chip, other), device_id_type=MESH,
        )
        f_copies[g, d].start()

    def spread(g):
        expect(g, b_rsem.at[g]).wait_recv()
        block = here.at[:, groups[g]]
        for d in order:
            for side in range(g + 1):
                g_copies[g, d, side] = pltpu.make_async_remote_copy(
                    src_ref=block, dst_ref=block, send_sem=g_ssem.at[g + side, d], recv_sem=g_rsem.at[g + side, d],
                    device_id={"ep": chip * 2 + (other if side else core), "tp": peer(d)}, device_id_type=MESH,
                )
                g_copies[g, d, side].start()
        forward(g, 0)

    def take(blocks, d, old):
        lane_group = peer(n_tp - d) if d else tp
        parts = [from_blocks(rows.at[lane_group, other if side else core].at[:, groups[g]]) for g, side in blocks]
        x = (parts[0] if len(parts) == 1 else jnp.concatenate(parts, axis=0)).astype(F32)
        columns = pl.ds(pl.multiple_of(lane_group * width, 128), width)
        part = jnp.sum(x * x, axis=-1, keepdims=True)
        y_rows = (x * norm_mid[:, columns]).astype(BF16)
        new = (part, dot_cols(y_rows, gate[0, :, columns]), dot_cols(y_rows, up[0, :, columns]))
        return new if old is None else tuple(m + n for m, n in zip(old, new))

    def finish(sums):
        squares, g_sum, u_sum = sums
        scale = lax.rsqrt(squares * (1.0 / (n_tp * width)) + EPS)
        gated = g_sum * scale
        return (gated / (1.0 + jnp.exp(-gated)) * (u_sum * scale)).astype(BF16)

    spread(0)
    l_norm_mid.wait()
    l_gate.wait()
    l_up.wait()
    first = take([(0, 0)], 0, None)
    spread(1)
    f_copies[0, 0].wait_recv()
    f_copies[1, 0].wait_recv()
    others = take([(0, 1), (1, 1), (1, 0)], 0, None)
    for d in (1, 3, 2):
        g_copies[0, d, 0].wait_recv()
        forward(0, d)
        first = take([(0, 0)], d, first)
    for d in (1, 3, 2):
        g_copies[1, d, 0].wait_recv()
        g_copies[1, d, 1].wait_recv()
        f_copies[0, d].wait_recv()
        others = take([(0, 1), (1, 1), (1, 0)], d, others)
    l_down.wait()
    d_copies, x_copies, totals = {}, {}, {}

    hidden = jnp.concatenate([finish(others), finish(first)], axis=0)
    n_near, n_far = 2 * near, 2 * (chips - near)
    near_span, far_span = pl.ds(0, n_near), pl.ds(n_near, n_far)
    def quarter(d):
        return dot(hidden, down[0, :, pl.ds(pl.multiple_of(peer(d) * width, 128), width)])

    n_all = n_near + n_far
    products = {d: quarter(d) for d in (2, 1)}
    for d in (2, 1, 3, 0):
        if d == 3:
            products.update({each: quarter(each) for each in (3, 0)})
        product = products[d]
        d_send[d] = product[:n_all].astype(BF16)
        d_copies[d] = pltpu.make_async_remote_copy(
            src_ref=d_send.at[d], dst_ref=d_recv.at[d], send_sem=d_ssem.at[d], recv_sem=d_rsem.at[d],
            device_id=ep_id(chip, other), device_id_type=MESH,
        )
        d_copies[d].start()
        own[d, far_span] = product[n_all : n_all + n_far]
        own[d, near_span] = product[n_all + n_far :]

    def across(g, d, span):
        x_send[d, span] = (own[d, span] + d_recv[d, span].astype(F32)).astype(BF16)
        x_copies[g, d] = pltpu.make_async_remote_copy(
            src_ref=x_send.at[d, span], dst_ref=x_recv.at[d, span],
            send_sem=x_ssem.at[g, d], recv_sem=x_rsem.at[g, d], device_id=tp_id(d), device_id_type=MESH,
        )
        x_copies[g, d].start()

    for d in order:
        d_copies[d].wait_recv()
        across(1, d, far_span)
    for d in order:
        across(0, d, near_span)
    d_copies[0].wait_recv()
    for g, span in enumerate((near_span, far_span)):
        totals[g] = own[0, span] + d_recv[0, span].astype(F32)

    def give_back(g):
        span = (near_span, far_span)[g]
        total = totals[g]
        for d in (1, 3, 2):
            x_copies[g, d].wait_recv()
            total = total + x_recv[d, span].astype(F32)
        for h, part in enumerate(to_blocks(total.astype(BF16))):
            e_send[h, groups[g]] = part
        for p in range(groups[g].start + groups[g].size - 1, max(0, groups[g].start - 1), -1):
            pltpu.make_async_remote_copy(
                src_ref=e_send.at[:, p], dst_ref=e_recv.at[:, chip], send_sem=e_ssem, recv_sem=e_rsem,
                device_id=ep_id(source(p), core), device_id_type=MESH,
            ).start()

    give_back(1)
    give_back(0)
    for h in range(2):
        e_recv[h, chip] = e_send[h, 0]
    rest = pl.ds(1, chips - 1)
    all_back = pltpu.make_async_remote_copy(
        src_ref=e_send.at[:, rest], dst_ref=e_recv.at[:, rest], send_sem=e_ssem, recv_sem=e_rsem,
        device_id=tp_id(1), device_id_type=MESH,
    )
    all_back.wait_recv()
    back = from_blocks(e_recv)
    mix = dot(combine_high, back) + dot(combine_low, back)
    out_ref[...] = (resid.astype(F32) + mix).astype(BF16)

    pltpu.make_async_remote_copy(
        src_ref=b_send.at[:, rest], dst_ref=here.at[:, rest], send_sem=b_ssem, recv_sem=b_rsem.at[0],
        device_id=tp_id(1), device_id_type=MESH,
    ).wait_send()
    all_back.wait_send()
    for d in order:
        a_copies[d].wait_send()
    for copies in (g_copies, f_copies, d_copies, x_copies):
        for copy in copies.values():
            copy.wait_send()


def body(
    n_ep, n_tp, tokens, seq_length, ret_state, norm_in, w_query, w_key, w_value, head_gain, w_output,
    norm_mid, route_expert, route_score, expert_gate, expert_up, expert_down,
):
    n_rows, model = tokens.shape
    chips = n_ep // 2
    width = model // n_tp
    args = (
        tokens, seq_length.reshape(1, -1), norm_in.reshape(1, -1), w_query, w_key, w_value, ret_state,
        head_gain.reshape(1, -1), w_output, norm_mid.reshape(1, -1), route_expert.T, route_score.T,
        expert_gate.swapaxes(1, 2), expert_up.swapaxes(1, 2), expert_down,
    )
    dma = pltpu.SemaphoreType.DMA
    blocks = (2, chips, 2, width // 2)
    held = [jax.ShapeDtypeStruct((model, 512), BF16) if a is w_query else a for a in args if a is not w_key and a is not w_value]
    scratch = [pltpu.VMEM(a.shape, a.dtype) for a in held] + [
        pltpu.VMEM((n_rows, head_gain.shape[0]), F32),
        pltpu.VMEM((n_tp, n_rows, width), BF16),
        pltpu.VMEM((n_tp, n_rows, width), BF16),
        pltpu.VMEM(blocks, BF16),
        pltpu.VMEM((n_tp, 2) + blocks, BF16),
        pltpu.VMEM((n_tp, 2 * chips, width), F32),
        pltpu.VMEM((n_tp, 2 * chips, width), BF16),
        pltpu.VMEM((n_tp, 2 * chips, width), BF16),
        pltpu.VMEM((n_tp, 2 * chips, width), BF16),
        pltpu.VMEM((n_tp, 2 * chips, width), BF16),
        pltpu.VMEM(blocks, BF16),
        pltpu.VMEM(blocks, BF16),
        dma((len(args) + 2,)),
        pltpu.SemaphoreType.REGULAR,
        dma((n_tp,)), dma((n_tp,)),
        dma, dma((2,)),
        dma((3, n_tp)), dma((3, n_tp)),
        dma((2, n_tp)), dma((2, n_tp)),
        dma((n_tp,)), dma((n_tp,)),
        dma((2, n_tp)), dma((2, n_tp)),
        dma, dma,
    ]
    return pl.pallas_call(
        functools.partial(kernel, n_ep, n_tp),
        out_shape=jax.ShapeDtypeStruct((n_rows, width), BF16),
        in_specs=[pl.BlockSpec(memory_space=pl.ANY)] * len(args),
        out_specs=pl.BlockSpec(memory_space=pltpu.VMEM),
        scratch_shapes=scratch,
        compiler_params=pltpu.CompilerParams(collective_id=0, has_side_effects=True, vmem_limit_bytes=40 << 20),
        name="step",
    )(*[pltpu.with_memory_space_constraint(a, pltpu.HBM) for a in args])


def solution(mesh):
    placed = (
        P("ep", None),
        P("ep"),
        P("ep", "tp", None, None),
        P(),
        P(None, "tp"),
        P(None, "tp"),
        P(None, "tp"),
        P("tp"),
        P("tp", None),
        P(),
        P("ep", None),
        P("ep", None),
        P("ep", None, "tp"),
        P("ep", None, "tp"),
        P("ep", "tp", None),
    )
    step = functools.partial(body, mesh.shape["ep"], mesh.shape["tp"])
    return jax.shard_map(step, mesh=mesh, in_specs=placed, out_specs=P("ep", "tp"), check_vma=False)
```

```python
import functools

import jax
import jax.numpy as jnp
from jax import lax
from jax.experimental import pallas as pl
from jax.experimental.pallas import tpu as pltpu
from jax.sharding import PartitionSpec as P

EPS = 1e-06
MESH = pl.DeviceIdType.MESH
F32 = jnp.float32
BF16 = jnp.bfloat16


def dot(a, b):
    return jnp.dot(a, b, preferred_element_type=F32)


def dot_cols(a, b):
    return lax.dot_general(a, b, (((1,), (1,)), ((), ())), preferred_element_type=F32)


def dot_rows(a, b):
    return lax.dot_general(a, b, (((0,), (0,)), ((), ())), preferred_element_type=F32)


def split(x):
    high = x.astype(BF16)
    return high, (x - high.astype(F32)).astype(BF16)


def to_blocks(x):
    rows = x.shape[0]
    return [x[:, 128 * h : 128 * (h + 1)].reshape(rows // 2, 2, 128) for h in range(2)]


def from_blocks(ref):
    blocks = ref.shape[0]
    return jnp.concatenate([ref[:, h].reshape(2 * blocks, 128) for h in range(2)], axis=1)


def ring_order(n_z, n_y):
    def hops(d):
        return min(d[0], n_z - d[0]) + min(d[1], n_y - d[1])

    return sorted(((dz, dy) for dz in range(n_z) for dy in range(n_y)), key=hops)


def kernel(
    n_ep,
    n_tp,
    tokens_h, seq_h, norm_in_h, wq_h, wk_h, wv_h, state_h, gain_h, wo_h, norm_mid_h,
    route_h, score_h, gate_h, up_h, down_h,
    out_ref,
    tokens, seq, norm_in, w_qkv, state, gain, wo, norm_mid, route, score, gate_up, down,
    carried, a_send, a_recv, b_send, rows, own, d_send, d_recv, x_send, x_recv, e_send, e_recv,
    load_sem, line_sem, a_ssem, a_rsem, b_ssem, b_rsem, g_ssem, g_rsem, f_ssem, f_rsem, d_ssem, d_rsem,
    x_ssem, x_rsem, e_ssem, e_rsem,
):
    chips = n_ep // 2
    ep = lax.axis_index("ep")
    tp = lax.axis_index("tp")
    chip = lax.div(ep, 2)
    core = lax.rem(ep, 2)
    other = 1 - core

    def peer(d):
        return lax.rem(tp + d, n_tp)

    n_y = 8 if chips % 8 == 0 else 2
    n_z = chips // n_y
    z = lax.div(chip, n_y)
    y = lax.rem(chip, n_y)
    offsets = ring_order(n_z, n_y)
    near = chips * 5 // 8

    def ahead(dz, dy):
        return lax.rem(z + dz, n_z) * n_y + lax.rem(y + dy, n_y)

    def target(p):
        return ahead(*offsets[p])

    def source(p):
        dz, dy = offsets[p]
        return ahead(n_z - dz, n_y - dy)

    def ep_id(c, co):
        return {"ep": c * 2 + co, "tp": tp}

    def tp_id(d):
        return {"ep": ep, "tp": peer(d)}

    sources = (tokens_h, seq_h, norm_in_h, wq_h, wk_h, wv_h, state_h, gain_h, wo_h, norm_mid_h,
               route_h, score_h, gate_h, up_h, down_h)
    places = (tokens, seq, norm_in, w_qkv.at[:, :128], w_qkv.at[:, 128:256], w_qkv.at[:, 256:], state, gain, wo, norm_mid, route, score, gate_up.at[pl.ds(0, 1)], gate_up.at[pl.ds(1, 1)], down)
    def load(i, sem):
        return pltpu.make_async_copy(sources[i], places[i], load_sem.at[sem])

    l_tokens, l_seq, l_norm_in, l_wq, l_wk, l_wv = [load(i, sem) for i, sem in enumerate((0, 1, 2, 3, 3, 3))]
    l_gain, l_wo, l_norm_mid, l_route, l_score = [load(i, sem) for i, sem in ((7, 6), (8, 7), (9, 0), (10, 1), (11, 2))]
    l_gate, l_up, l_down = load(12, 3), load(13, 3), load(14, 4)
    l_qkv = pltpu.make_async_copy(w_qkv, w_qkv, load_sem.at[3])
    l_gate_up = pltpu.make_async_copy(gate_up, gate_up, load_sem.at[3])
    n_half = tokens.shape[0] // 2
    l_states = [
        pltpu.make_async_copy(state_h.at[half], state.at[half], load_sem.at[4 + i])
        for i, half in enumerate((pl.ds(0, n_half), pl.ds(n_half, n_half)))
    ]
    for each in (l_tokens, l_norm_in, l_seq, l_wq, l_wk, l_wv):
        each.start()

    barrier = pltpu.get_barrier_semaphore()

    lines = [ahead(0, d) for d in range(1, n_y)] + [ahead(d, 0) for d in range(1, n_z)]
    for c in lines:
        pl.semaphore_signal(barrier, inc=1, device_id=ep_id(c, core), device_id_type=MESH)
    for d in range(1, n_tp):
        pl.semaphore_signal(barrier, inc=1, device_id=tp_id(d), device_id_type=MESH)
    pl.semaphore_signal(barrier, inc=1, device_id=ep_id(chip, other), device_id_type=MESH)

    for each in (*l_states, l_gain, l_wo):
        each.start()
    l_tokens.wait()
    l_norm_in.wait()
    l_seq.wait()
    token_f = tokens[...].astype(F32)
    row_scale = lax.rsqrt(jnp.mean(token_f * token_f, axis=-1, keepdims=True) + EPS)
    n_rows = token_f.shape[0]
    sub = lax.broadcasted_iota(jnp.int32, (n_rows, n_rows), 0)
    lane = lax.broadcasted_iota(jnp.int32, (n_rows, n_rows), 1)

    def column(row):
        return jnp.sum(jnp.where(sub == lane, row.astype(F32), 0.0), axis=1, keepdims=True)

    positions = column(seq[...])
    key_lane = lax.broadcasted_iota(jnp.int32, (n_rows, 128), 1)
    pair = lax.rem(key_lane, 64).astype(F32)
    angles = positions * jnp.exp(pair * (-jnp.log(10000.0) / 64.0))
    cosine = jnp.cos(angles)
    sine = jnp.where(key_lane < 64, -1.0, 1.0) * jnp.sin(angles)

    def rotate(x):
        return x * cosine + pltpu.roll(x, 64, 1) * sine

    gained = (token_f * norm_in[...]).astype(BF16)
    l_qkv.wait()
    projected = dot(gained, w_qkv[...]) * row_scale
    q_rot = rotate(projected[:, :128])
    k_rot = rotate(projected[:, 128:256]) * (128.0 ** -0.5)
    value_rows = projected[:, 256:]
    within = jnp.sum(q_rot * k_rot, axis=-1, keepdims=True) * value_rows
    q_cols = q_rot.T
    for b in range(n_rows):
        if b % (n_rows // 2) == 0:
            l_states[b // (n_rows // 2)].wait()
        carried[b : b + 1, :] = jnp.sum(q_cols[:, b : b + 1] * state[b, 0], axis=0, keepdims=True)
    for each in (l_route, l_score, l_norm_mid, l_gate, l_up, l_down):
        each.start()
    head = jnp.full((1, 1), tp, jnp.int32).astype(F32)
    decay = 1.0 - jnp.exp2(-2.0 - 2.0 * head)
    retained = decay * carried[...] + within
    centred = retained - jnp.mean(retained, axis=-1, keepdims=True)
    variance = jnp.mean(centred * centred, axis=-1, keepdims=True)
    l_gain.wait()
    ret_out = (centred * lax.rsqrt(variance + EPS) * gain[...]).astype(BF16)
    l_wo.wait()
    width = out_ref.shape[1]
    mine = pl.ds(pl.multiple_of(tp * width, 128), width)

    order = [2, 1, 3]
    for d in order:
        columns = pl.ds(pl.multiple_of(peer(d) * width, 128), width)
        a_send[d] = dot(ret_out, wo[:, columns]).astype(BF16)
    own_part = dot(ret_out, wo[:, mine]).astype(BF16).astype(F32)

    pl.semaphore_wait(barrier, n_tp + len(lines))
    for d in range(1, n_z):
        pl.semaphore_signal(line_sem, inc=1, device_id=ep_id(ahead(d, 0), core), device_id_type=MESH)
    a_copies = {}
    for d in order:
        a_copies[d] = pltpu.make_async_remote_copy(
            src_ref=a_send.at[d], dst_ref=a_recv.at[d], send_sem=a_ssem, recv_sem=a_rsem,
            device_id=tp_id(d), device_id_type=MESH,
        )
        a_copies[d].start()

    l_route.wait()
    l_score.wait()
    experts = chips
    expert_lane = lax.broadcasted_iota(jnp.int32, (n_rows, 2 * experts), 1)
    choice = [column(route[k : k + 1, :]).astype(jnp.int32) for k in range(2)]
    named = [(expert_lane == c).astype(F32) for c in choice]
    earlier = dot((lane < sub).astype(BF16), (named[0] + named[1]).astype(BF16))
    picked = []
    for k in range(2):
        rank = jnp.sum(earlier * named[k], axis=1, keepdims=True).astype(jnp.int32)
        picked.append((expert_lane == choice[k] * 2 + rank).astype(F32))
    placing = (picked[0] + picked[1]).astype(BF16)
    grown = jnp.exp(score[...] - jnp.max(score[...], axis=0, keepdims=True))
    weights = grown / jnp.sum(grown, axis=0, keepdims=True)
    combine = picked[0] * column(weights[0:1, :]) + picked[1] * column(weights[1:2, :])
    combine_high, combine_low = split(combine)


    attended = own_part
    a_all = pltpu.make_async_remote_copy(
        src_ref=a_send.at[pl.ds(1, n_tp - 1)], dst_ref=a_recv.at[pl.ds(1, n_tp - 1)], send_sem=a_ssem, recv_sem=a_rsem,
        device_id=tp_id(1), device_id_type=MESH,
    )
    a_all.wait_recv()
    for d in (1, 3, 2):
        attended = attended + a_recv[d].astype(F32)
    resid = (tokens[:, mine].astype(F32) + attended).astype(BF16)

    packed = dot_rows(placing, resid).astype(BF16)
    for h, part in enumerate(to_blocks(packed)):
        b_send[:, h] = part

    here = rows.at[tp, core]
    groups = (pl.ds(0, near), pl.ds(near, chips - near))
    pl.semaphore_wait(line_sem, n_z - 1)
    for p in range(chips - 1, 0, -1):
        far = target(p)
        pltpu.make_async_remote_copy(
            src_ref=b_send.at[far], dst_ref=here.at[p], send_sem=b_ssem, recv_sem=b_rsem.at[int(p >= near)],
            device_id=ep_id(far, core), device_id_type=MESH,
        ).start()
    rows[tp, core, 0] = b_send[chip]

    def expect(group, recv_sem):
        first, size = ((1, near - 1), (near, chips - near))[group]
        block = here.at[pl.ds(first, size)]
        return pltpu.make_async_remote_copy(
            src_ref=block, dst_ref=block, send_sem=b_ssem, recv_sem=recv_sem, device_id=tp_id(1), device_id_type=MESH,
        )

    g_copies, f_copies = {}, {}

    def forward(g, d):
        block = rows.at[peer(n_tp - d) if d else tp, core].at[groups[g]]
        f_copies[g, d] = pltpu.make_async_remote_copy(
            src_ref=block, dst_ref=block, send_sem=f_ssem.at[g], recv_sem=f_rsem.at[n_tp * g + d],
            device_id=ep_id(chip, other), device_id_type=MESH,
        )
        f_copies[g, d].start()

    def spread(g):
        expect(g, b_rsem.at[g]).wait_recv()
        block = here.at[groups[g]]
        for d in order:
            for side in range(g + 1):
                g_copies[g, d, side] = pltpu.make_async_remote_copy(
                    src_ref=block, dst_ref=block, send_sem=g_ssem.at[g], recv_sem=g_rsem.at[g, d],
                    device_id={"ep": chip * 2 + (other if side else core), "tp": peer(d)}, device_id_type=MESH,
                )
                g_copies[g, d, side].start()
        forward(g, 0)

    def take(blocks, d, old):
        lane_group = peer(n_tp - d) if d else tp
        parts = [from_blocks(rows.at[lane_group, other if side else core].at[groups[g]]) for g, side in blocks]
        x = (parts[0] if len(parts) == 1 else jnp.concatenate(parts, axis=0)).astype(F32)
        columns = pl.ds(pl.multiple_of(lane_group * width, 128), width)
        part = jnp.sum(x * x, axis=-1, keepdims=True)
        y_rows = (x * norm_mid[:, columns]).astype(BF16)
        new = (part, dot_cols(y_rows, gate_up[0, :, columns]), dot_cols(y_rows, gate_up[1, :, columns]))
        return new if old is None else tuple(m + n for m, n in zip(old, new))

    def finish(sums):
        squares, g_sum, u_sum = sums
        scale = lax.rsqrt(squares * (1.0 / (n_tp * width)) + EPS)
        gated = g_sum * scale
        return (gated / (1.0 + jnp.exp(-gated)) * (u_sum * scale)).astype(BF16)

    spread(0)
    l_norm_mid.wait()
    l_gate_up.wait()
    first = take([(0, 0)], 0, None)
    spread(1)
    f_copies[0, 0].wait_recv()
    f_copies[1, 0].wait_recv()
    others = take([(0, 1), (1, 1), (1, 0)], 0, None)
    for d in (1, 3, 2):
        g_copies[0, d, 0].wait_recv()
        forward(0, d)
        first = take([(0, 0)], d, first)
    for d in (1, 3, 2):
        block = rows.at[peer(n_tp - d), :, groups[1]]
        pltpu.make_async_remote_copy(
            src_ref=block, dst_ref=block, send_sem=g_ssem.at[1], recv_sem=g_rsem.at[1, d], device_id=tp_id(d), device_id_type=MESH,
        ).wait_recv()
        f_copies[0, d].wait_recv()
        others = take([(0, 1), (1, 1), (1, 0)], d, others)
    l_down.wait()
    d_copies, x_copies = {}, {}

    hidden = jnp.concatenate([finish(others), finish(first)], axis=0)
    n_near, n_far = 2 * near, 2 * (chips - near)
    near_span, far_span = pl.ds(0, n_near), pl.ds(n_near, n_far)
    def quarter(d):
        return dot(hidden, down[0, :, pl.ds(pl.multiple_of(peer(d) * width, 128), width)])

    n_all = n_near + n_far
    products = {d: quarter(d) for d in (2, 1)}
    for d in (2, 1, 3, 0):
        if d == 3:
            products.update({each: quarter(each) for each in (3, 0)})
        product = products[d]
        d_send[d] = product[:n_all].astype(BF16)
        d_copies[d] = pltpu.make_async_remote_copy(
            src_ref=d_send.at[d], dst_ref=d_recv.at[d], send_sem=d_ssem, recv_sem=d_rsem.at[d],
            device_id=ep_id(chip, other), device_id_type=MESH,
        )
        d_copies[d].start()
        own[d, far_span] = product[n_all : n_all + n_far]
        own[d, near_span] = product[n_all + n_far :]

    def across(g, d, span):
        x_send[d, span] = (own[d, span] + d_recv[d, span].astype(F32)).astype(BF16)
        x_copies[g, d] = pltpu.make_async_remote_copy(
            src_ref=x_send.at[d, span], dst_ref=x_recv.at[d, span],
            send_sem=x_ssem, recv_sem=x_rsem.at[g], device_id=tp_id(d), device_id_type=MESH,
        )
        x_copies[g, d].start()

    cuts = (0, 3 * chips // 8, 3 * chips // 4, chips)
    returns = [pl.ds(low, high - low) for low, high in zip(cuts, cuts[1:])]
    spans = [pl.ds(2 * part.start, 2 * part.size) for part in returns]
    for d in order:
        d_copies[d].wait_recv()
        across(2, d, spans[2])
    for g in (1, 0):
        for d in order:
            across(g, d, spans[g])
    d_copies[0].wait_recv()

    def give_back(g):
        span, group = spans[g], returns[g]
        total = own[0, span] + d_recv[0, span].astype(F32)
        others_here = x_recv.at[pl.ds(1, n_tp - 1), span]
        pltpu.make_async_remote_copy(
            src_ref=others_here, dst_ref=others_here, send_sem=x_ssem, recv_sem=x_rsem.at[g], device_id=tp_id(1), device_id_type=MESH,
        ).wait_recv()
        for d in (1, 3, 2):
            total = total + x_recv[d, span].astype(F32)
        for h, part in enumerate(to_blocks(total.astype(BF16))):
            e_send[group, h] = part
        for p in range(group.start + group.size - 1, max(0, group.start - 1), -1):
            pltpu.make_async_remote_copy(
                src_ref=e_send.at[p], dst_ref=e_recv.at[chip], send_sem=e_ssem, recv_sem=e_rsem,
                device_id=ep_id(source(p), core), device_id_type=MESH,
            ).start()

    for g in (2, 1, 0):
        give_back(g)
    e_recv[chip] = e_send[0]
    rest = pl.ds(1, chips - 1)
    all_back = pltpu.make_async_remote_copy(
        src_ref=e_send.at[rest], dst_ref=e_recv.at[rest], send_sem=e_ssem, recv_sem=e_rsem,
        device_id=tp_id(1), device_id_type=MESH,
    )
    all_back.wait_recv()
    back = from_blocks(e_recv)
    mix = dot(combine_high, back) + dot(combine_low, back)
    out_ref[...] = (resid.astype(F32) + mix).astype(BF16)

    pltpu.make_async_remote_copy(
        src_ref=b_send.at[rest], dst_ref=here.at[rest], send_sem=b_ssem, recv_sem=b_rsem.at[0],
        device_id=tp_id(1), device_id_type=MESH,
    ).wait_send()
    all_back.wait_send()
    a_all.wait_send()
    three = pl.ds(0, n_tp - 1)
    for block, sem in (
        (rows.at[three, core, groups[0]], g_ssem.at[0]),
        (rows.at[three, :, groups[1]], g_ssem.at[1]),
        (rows.at[:, core, groups[0]], f_ssem.at[0]),
        (here.at[groups[1]], f_ssem.at[1]),
        (d_send, d_ssem),
        (x_send.at[three], x_ssem),
    ):
        pltpu.make_async_remote_copy(
            src_ref=block, dst_ref=block, send_sem=sem, recv_sem=sem, device_id=tp_id(1), device_id_type=MESH
        ).wait_send()


def body(
    n_ep, n_tp, tokens, seq_length, ret_state, norm_in, w_query, w_key, w_value, head_gain, w_output,
    norm_mid, route_expert, route_score, expert_gate, expert_up, expert_down,
):
    n_rows, model = tokens.shape
    chips = n_ep // 2
    width = model // n_tp
    args = (
        tokens, seq_length.reshape(1, -1), norm_in.reshape(1, -1), w_query, w_key, w_value, ret_state,
        head_gain.reshape(1, -1), w_output, norm_mid.reshape(1, -1), route_expert.T, route_score.T,
        expert_gate.swapaxes(1, 2), expert_up.swapaxes(1, 2), expert_down,
    )
    dma = pltpu.SemaphoreType.DMA
    blocks = (chips, 2, 2, width // 2)
    held = list(args)
    held[3:6] = [jax.ShapeDtypeStruct((model, 512), BF16)]
    held[10:12] = [jax.ShapeDtypeStruct((2,) + args[12].shape[1:], BF16)]
    scratch = [pltpu.VMEM(a.shape, a.dtype) for a in held] + [
        pltpu.VMEM((n_rows, head_gain.shape[0]), F32),
        pltpu.VMEM((n_tp, n_rows, width), BF16),
        pltpu.VMEM((n_tp, n_rows, width), BF16),
        pltpu.VMEM(blocks, BF16),
        pltpu.VMEM((n_tp, 2) + blocks, BF16),
        pltpu.VMEM((n_tp, 2 * chips, width), F32),
        pltpu.VMEM((n_tp, 2 * chips, width), BF16),
        pltpu.VMEM((n_tp, 2 * chips, width), BF16),
        pltpu.VMEM((n_tp, 2 * chips, width), BF16),
        pltpu.VMEM((n_tp, 2 * chips, width), BF16),
        pltpu.VMEM(blocks, BF16),
        pltpu.VMEM(blocks, BF16),
        dma((8,)),
        pltpu.SemaphoreType.REGULAR,
        dma, dma,
        dma, dma((2,)),
        dma((2,)), dma((2, n_tp)),
        dma((2,)), dma((n_tp + 1,)),
        dma, dma((n_tp,)),
        dma, dma((3,)),
        dma, dma,
    ]
    return pl.pallas_call(
        functools.partial(kernel, n_ep, n_tp),
        out_shape=jax.ShapeDtypeStruct((n_rows, width), BF16),
        in_specs=[pl.BlockSpec(memory_space=pl.ANY)] * len(args),
        out_specs=pl.BlockSpec(memory_space=pltpu.VMEM),
        scratch_shapes=scratch,
        compiler_params=pltpu.CompilerParams(collective_id=0, has_side_effects=True, vmem_limit_bytes=40 << 20),
        name="step",
    )(*[pltpu.with_memory_space_constraint(a, pltpu.HBM) for a in args])


def solution(mesh):
    placed = (
        P("ep", None),
        P("ep"),
        P("ep", "tp", None, None),
        P(),
        P(None, "tp"),
        P(None, "tp"),
        P(None, "tp"),
        P("tp"),
        P("tp", None),
        P(),
        P("ep", None),
        P("ep", None),
        P("ep", None, "tp"),
        P("ep", None, "tp"),
        P("ep", "tp", None),
    )
    step = functools.partial(body, mesh.shape["ep"], mesh.shape["tp"])
    return jax.shard_map(step, mesh=mesh, in_specs=placed, out_specs=P("ep", "tp"), check_vma=False)
```
